32 devices in a mesh: kv: 16 (over z, x, core), tp: 2 (over y).
Axes of the slice: x: 2, y: 2, z: 4, core: 2. Of those that a mesh axis runs over, the one named last changes fastest.
Arguments:
- queries: bfloat16 [2048, 4096], P('kv', 'tp'), may hold values from -6 to 6
- keys: bfloat16 [2048, 512], P('kv', 'tp'), may hold values from -6 to 6
- values: bfloat16 [2048, 512], P('kv', 'tp'), may hold values from -6 to 6
- logsum: float32 [2048, 32], P('kv', 'tp'), may hold values from 2 to 6
- out_grad: bfloat16 [2048, 4096], P('kv', 'tp'), may hold values from -6 to 6
- normed_input: bfloat16 [2048, 4096], P('kv', 'tp'), may hold values from -6 to 6
- chosen: int32 [32, 16], P('kv'), may hold values from 0 to 63, as said below
Outputs:
- query_grad: float32 [2048, 4096], P('kv', 'tp')
- key_grad: float32 [2048, 512], P('kv', 'tp')
- value_grad: float32 [2048, 512], P('kv', 'tp')
- value_weight_grad: float32 [4096, 512], P('kv', 'tp')
The draws below stay inside these ranges and needn't reach their ends.
Inputs may be any that keep to these rules, and one draw needn't show every extreme that they name: `chosen`: each row r names 16 distinct key blocks, among them block 0 and the blocks r * 2 to r * 2 + 64 / 32 - 1 that hold the query block's own positions. The rows of one device (aligned runs of 2 rows) name at most one block of any other device's 128 / 32 blocks. Blocks after the query block may be named; their keys are masked.
All inputs are finite; a program needn't handle non-finite values.
Results may differ from the reference program's by a relative error of at most 0.008.
Values may be sent and summed in bfloat16 or wider, within the bound.
A program may use at most 64 MiB of HBM per device.

```python
import jax
import jax.numpy as jnp
from jax import lax

D = 4096
HEADS = 32
KV_HEADS = 4
HD = 128
TOK_DEV = 128
QB = 64
KB = 32
NSEL = 16
TOKENS = 2048


def draw_chosen(key, part):
    kblock_count = TOK_DEV // KB
    qblock_count = TOK_DEV // QB
    devices = TOKENS // TOK_DEV
    row_count = TOKENS // QB
    diag = QB // KB
    ncand = devices + kblock_count
    key_pick = jax.random.fold_in(key, 11)
    key_pop = jax.random.fold_in(key, 12)
    key_far = jax.random.fold_in(key, 13)
    key_own = jax.random.fold_in(key, 14)
    owners = jnp.arange(devices, dtype=jnp.int32)
    pick = jax.random.randint(key_pick, (devices, devices), 0, kblock_count)
    pick = jnp.where(owners[None, :] == 0, 0, pick)
    popular = jax.random.randint(key_pop, (devices,), 0, 8)
    rows = jnp.arange(row_count, dtype=jnp.int32)
    device_of = rows // qblock_count
    first = rows * diag
    remote_blk = owners[None, :] * kblock_count + pick[device_of]
    own_blk = device_of[:, None] * kblock_count + jnp.arange(kblock_count, dtype=jnp.int32)[None, :]
    cand = jnp.concatenate([remote_blk, own_blk], axis=1)
    cand_owner = cand // kblock_count
    slot_owner = jnp.concatenate([owners, jnp.full((kblock_count,), -1, jnp.int32)])
    is_diag = (cand >= first[:, None]) & (cand < first[:, None] + diag)
    invalid = (slot_owner[None, :] == device_of[:, None]) | is_diag
    forced = (cand == 0) | (cand_owner == device_of[:, None] - 1) | (cand_owner == device_of[:, None] - devices // 2)
    causal = cand < first[:, None]
    far_noise = jax.random.randint(key_far, (row_count, devices), 0, 32) + popular[None, :]
    own_noise = jax.random.randint(key_own, (row_count, kblock_count), 0, 32)
    noise = jnp.concatenate([far_noise, own_noise], axis=1)
    tier = jnp.where(forced, 3, jnp.where(causal, 2, 1))
    index = jnp.arange(ncand, dtype=jnp.int32)[None, :]
    score = jnp.where(invalid, 0, tier * 64 + noise) * ncand + (ncand - 1 - index)
    _, top = lax.top_k(score, NSEL - diag)
    picked = jnp.take_along_axis(cand, top, axis=1)
    diag_ids = first[:, None] + jnp.arange(diag, dtype=jnp.int32)[None, :]
    return jnp.concatenate([diag_ids, picked], axis=1).astype(jnp.int32)


def block_levels(stream_key, extent, split, least, high):
    loudness, own = 1.0, jax.random.fold_in(stream_key, 6)
    for position, blocks in split:
        steps = jnp.exp(jax.random.uniform(jax.random.fold_in(own, position), (blocks,), jnp.float32, least / len(split), high / len(split)))
        loudness = loudness * jnp.repeat(steps, extent[position] // blocks).reshape([-1 if axis == position else 1 for axis in range(len(extent))])
    return loudness


def bell_draw(stream_key, dims, width, limit, shards=(), kind=jnp.bfloat16):
    gain = block_levels(stream_key, dims, shards, -0.22, 0.18) if shards else 1.0
    drawn = jax.random.normal(stream_key, dims, jnp.float32) * width * gain
    return jnp.minimum(jnp.maximum(drawn, -limit), limit).astype(kind)


def setup_inputs(seed: int = 0) -> dict:
    streams_of = jax.random.split(jax.random.key(seed), 8)
    return {
        "queries": bell_draw(streams_of[0], (TOKENS, HEADS * HD), 1.0, 6.0, ((0, 16), (1, 2))),
        "keys": bell_draw(streams_of[1], (TOKENS, KV_HEADS * HD), 1.0, 6.0, ((0, 16), (1, 2))),
        "values": bell_draw(streams_of[2], (TOKENS, KV_HEADS * HD), 1.0, 6.0, ((0, 16), (1, 2))),
        "logsum": jnp.clip(2.0 + 4.0 * jax.random.uniform(streams_of[3], (TOKENS, HEADS), jnp.float32) ** block_levels(streams_of[3], (TOKENS, HEADS), ((0, 16), (1, 2)), -0.2, 0.2), 2.0, 6.0),
        "out_grad": bell_draw(streams_of[4], (TOKENS, HEADS * HD), 1.0, 6.0, ((0, 16), (1, 2))),
        "normed_input": bell_draw(streams_of[5], (TOKENS, D), 1.0, 6.0, ((0, 16), (1, 2))),
        "chosen": draw_chosen(jax.random.fold_in(streams_of[7], 71), 0),
    }


def reference(queries, keys, values, logsum, out_grad, normed_input, chosen):
    group = HEADS // KV_HEADS
    kv_cols = KV_HEADS * HD
    scale = HD ** -0.5
    blocks = TOKENS // KB
    key_blocks = keys.reshape(blocks, KB, KV_HEADS, HD)
    value_blocks = values.reshape(blocks, KB, KV_HEADS, HD)
    offsets = jnp.arange(KB, dtype=jnp.int32)
    rows_in = jnp.arange(QB, dtype=jnp.int32)

    def step(carry, index):
        key_acc, value_acc = carry
        ids = chosen[index]
        start = index * QB
        query_rows = lax.dynamic_slice_in_dim(queries, start, QB, 0).reshape(QB, KV_HEADS, group, HD).astype(jnp.float32)
        dout = lax.dynamic_slice_in_dim(out_grad, start, QB, 0).reshape(QB, KV_HEADS, group, HD).astype(jnp.float32)
        lse = lax.dynamic_slice_in_dim(logsum, start, QB, 0).reshape(QB, KV_HEADS, group)
        sel_keys = key_blocks[ids].reshape(NSEL * KB, KV_HEADS, HD).astype(jnp.float32)
        sel_values = value_blocks[ids].reshape(NSEL * KB, KV_HEADS, HD).astype(jnp.float32)
        scores = jnp.einsum("qngd,jnd->qngj", query_rows, sel_keys) * scale
        qpos = start + rows_in
        kpos = (ids[:, None] * KB + offsets[None, :]).reshape(NSEL * KB)
        valid = (kpos[None, :] <= qpos[:, None])[:, None, None, :]
        prob = jnp.where(valid, jnp.exp(scores - lse[..., None]), 0.0)
        dprob = jnp.einsum("qngd,jnd->qngj", dout, sel_values)
        delta = jnp.sum(prob * dprob, axis=-1, keepdims=True)
        dscore = lax.optimization_barrier((prob * (dprob - delta)).astype(jnp.bfloat16)).astype(jnp.float32)
        prob_low = lax.optimization_barrier(prob.astype(jnp.bfloat16)).astype(jnp.float32)
        query_part = jnp.einsum("qngj,jnd->qngd", dscore, sel_keys) * scale
        key_part = jnp.einsum("qngj,qngd->jnd", dscore, query_rows) * scale
        value_part = jnp.einsum("qngj,qngd->jnd", prob_low, dout)
        key_acc = key_acc.at[ids].add(key_part.reshape(NSEL, KB * kv_cols))
        value_acc = value_acc.at[ids].add(value_part.reshape(NSEL, KB * kv_cols))
        return (key_acc, value_acc), query_part.reshape(QB, HEADS * HD)

    zeros = jnp.zeros((blocks, KB * kv_cols), jnp.float32)
    (key_acc, value_acc), query_rows_all = lax.scan(step, (zeros, zeros), jnp.arange(TOKENS // QB, dtype=jnp.int32))
    query_grad = query_rows_all.reshape(TOKENS, HEADS * HD)
    key_grad = key_acc.reshape(TOKENS, kv_cols)
    value_grad = value_acc.reshape(TOKENS, kv_cols)
    value_low = value_grad.astype(jnp.bfloat16)
    weight_grad = jnp.dot(normed_input.astype(jnp.float32).T, value_low.astype(jnp.float32))
    return query_grad, key_grad, value_grad, weight_grad
```

```python
import functools

import jax
import jax.numpy as jnp
from jax import lax
from jax.experimental import pallas as pl
from jax.experimental.pallas import tpu as pltpu
from jax.sharding import PartitionSpec as P

HD = 128
QB = 64
KB = 32
NSEL = 16
FAR = 1e30
LOG2E = 1.4426950408889634

MESH = pl.DeviceIdType.MESH
F32 = jnp.float32
BF16 = jnp.bfloat16


def remote(src, dst, send_sem, recv_sem, device_id):
    return pltpu.make_async_remote_copy(
        src_ref=src,
        dst_ref=dst,
        send_sem=send_sem,
        recv_sem=recv_sem,
        device_id=device_id,
        device_id_type=MESH,
    )


def dot(a, b, dims):
    return lax.dot_general(a, b, (dims, ((), ())), preferred_element_type=F32)


def loop(first, last, body):
    def step(i, carry):
        body(i)
        return carry

    lax.fori_loop(first, last, step, 0)


def mark(name):
    pass


def kernel(
    n,
    tp,
    chosen_hbm,
    queries,
    keys,
    values,
    logsum,
    out_grad,
    normed_hbm,
    query_grad,
    key_grad,
    value_grad,
    weight_grad,
    chosen,
    q_all,
    do_all,
    logs,
    log2s,
    normed,
    pool,
    ask,
    asked,
    named,
    give,
    back_v,
    back_k,
    got_v,
    got_k,
    low_pool,
    norm_parts,
    norm_via,
    norm_pool,
    pen,
    pen_own,
    s_buf,
    dp,
    p_low,
    delta,
    dq_acc,
    in_sem,
    ask_send,
    ask_recv,
    out_send,
    kv_recv,
    bv_recv,
    bk_recv,
    via_send,
    via_recv,
    norm_send,
    norm_recv,
    swap_send,
    swap_recv,
    lo_send,
    lo_recv,
):
    me = lax.axis_index("kv")
    col = lax.axis_index("tp")
    kblocks = keys.shape[0]
    tok = kblocks * KB
    qblocks = tok // QB
    kv_cols = keys.shape[2]
    kv_heads = kv_cols // HD
    group = queries.shape[1] // kv_cols
    width = group * tok
    per = n // tp
    sub = norm_parts.shape[2]
    rows = sub * tp
    scale = HD ** (-0.5)
    xs = tp
    row = 2 * xs
    zs = n // row
    z = me // row
    r = me % row
    x = r // 2
    c = r % 2
    lanes = [slice(g * HD, (g + 1) * HD) for g in range(kv_heads)]

    barrier = pltpu.get_barrier_semaphore()

    mark("greet")

    def greet(i):
        pl.semaphore_signal(barrier, inc=1, device_id={"kv": i}, device_id_type=MESH)

    loop(0, n, greet)
    for d in range(1, tp):
        pl.semaphore_signal(
            barrier, inc=1, device_id={"tp": (col + d) % tp}, device_id_type=MESH
        )

    ins = [
        [pltpu.make_async_copy(chosen_hbm, chosen, in_sem.at[0])],
        [pltpu.make_async_copy(normed_hbm, normed, in_sem.at[1])],
        [
            pltpu.make_async_copy(ref, pool.at[pl.ds(n, kblocks), a], in_sem.at[2 + a])
            for a, ref in ((0, keys), (1, values))
        ],
        [pltpu.make_async_copy(logsum, logs, in_sem.at[4])],
    ]
    big = []
    for a, (src, dst) in enumerate(((queries, q_all), (out_grad, do_all))):
        for g in range(kv_heads):
            for h in range(group):
                at = (g * group + h) * HD
                big.append(
                    pltpu.make_async_copy(
                        src.at[:, at : at + HD],
                        dst.at[g, h * tok : (h + 1) * tok],
                        in_sem.at[5 + a],
                    )
                )
    for cs in ins:
        for cp in cs:
            cp.start()
    for cp in big:
        cp.start()

    mark("ask")
    for q in range(row):

        @pl.when(q >= r)
        def _():
            pool[z * row + q] = jnp.zeros_like(pool[z * row + q])

    ins[0][0].wait()
    lane = lax.broadcasted_iota(jnp.int32, (8, HD), 1)
    base = lane * kblocks
    wanted = jnp.zeros((8, HD), F32)
    missing = []
    missing_own = []
    for b in range(qblocks):
        far = jnp.full((8, HD), FAR, F32)
        far_own = jnp.full((8, HD), FAR, F32)
        for e in range(NSEL):
            block = chosen[b, e]
            at = block - base
            hit = (at >= 0) & (at < kblocks)
            wanted = jnp.where(hit, (at + 1).astype(F32), wanted)
            far = jnp.where(hit, 0.0, far)
            far_own = jnp.where(block - me * kblocks == lane, 0.0, far_own)
        missing.append(jnp.broadcast_to(far[:1], (QB, HD)))
        missing_own.append(jnp.broadcast_to(far_own[:1], (QB, HD)))
    ask[...] = wanted
    pen[...] = jnp.concatenate(missing, axis=0).T
    pen_own[...] = jnp.concatenate(missing_own, axis=0).T

    mark("turn")
    ins[1][0].wait()
    for m in range(normed.shape[1] // HD):
        turned = normed[:, m * HD : (m + 1) * HD].T
        for p in range(0, HD, sub):
            at = m * HD + p
            norm_parts[at % rows // sub, at // rows] = turned[p : p + sub]

    mark("barrier")
    pl.semaphore_wait(barrier, n + tp - 1)

    def place(i):
        return jnp.where(i // row == z, zs + i % row, i // row)

    mark("asksend")

    def ask_copy(i):
        return remote(ask, asked.at[me], ask_send.at[i], ask_recv.at[place_of_me(i)], {"kv": i})

    def place_of_me(i):
        return jnp.where(i // row == z, zs + r, z)

    loop(0, me, lambda i: ask_copy(i).start())

    def via_copy(d, k):
        q = (col + d) % tp
        return remote(
            norm_parts.at[q, k], norm_via.at[d, k], via_send.at[d], via_recv.at[d, k], {"tp": q}
        )

    for d in range(1, tp):
        loop(0, per, lambda k: via_copy(d, k).start())

    def norm_copy(d, k):
        t = (col + tp - d) % tp
        dest = t * per + k
        src = norm_parts.at[col, k] if d == 0 else norm_via.at[d, k]
        return remote(
            src, norm_pool.at[col, me], norm_send.at[0], norm_recv.at[place_of_me(dest)],
            {"kv": dest},
        )

    def norm_start(d, k, low):
        t = (col + tp - d) % tp
        dest = t * per + k

        if low:

            @pl.when(dest == me)
            def _():
                src = norm_parts[col, k] if d == 0 else norm_via[d, k]
                norm_pool[col, me] = src

            @pl.when((dest != me) & (dest // row <= z))
            def _():
                norm_copy(d, k).start()
        else:

            @pl.when(dest // row > z)
            def _():
                norm_copy(d, k).start()

    mark("normlow")
    loop(0, per, lambda k: norm_start(0, k, True))

    mark("own")
    for cp in ins[2] + ins[3]:
        cp.wait()
    for cp in big:
        cp.wait()
    for g in range(kv_heads):
        log2s[g] = jnp.concatenate(
            [logs[g * group + h : g * group + h + 1] * LOG2E for h in range(group)], axis=1
        )

    def take(a, first, count, g):
        return pool[pl.ds(first, count), a, :, lanes[g]].reshape(count * KB, HD)

    key_iota = lax.broadcasted_iota(jnp.int32, (KB, tok), 0)
    row_iota = lax.broadcasted_iota(jnp.int32, (KB, tok), 1)

    def early(first, count, own):
        for g in range(kv_heads):
            s_buf[: count * KB] = dot(take(0, first, count, g), q_all[g], ((1,), (1,)))
            dp[g, pl.ds(first, count)] = dot(
                take(1, first, count, g), do_all[g], ((1,), (1,))
            ).reshape(count, KB, width)
            total = jnp.zeros((8, width), F32) if own else delta[g]
            for u in range(count):
                if own:
                    gone = jnp.where(key_iota + u * KB <= row_iota, 0.0, FAR)
                    gone = gone + pen_own[u : u + 1]
                else:
                    gone = pen[pl.ds(first + u, 1)]
                bias = log2s[g] + jnp.concatenate([gone] * group, axis=1)
                p = jnp.exp2(s_buf[u * KB : (u + 1) * KB] * (scale * LOG2E) - bias)
                p_low[g, first + u] = p.astype(BF16)
                pd = p * dp[g, first + u]
                total = total + jnp.sum(pd.reshape(KB // 8, 8, width), axis=0)
            delta[g] = total
            dv = dot(
                p_low[g, pl.ds(first, count)].reshape(count * KB, width), do_all[g], ((1,), (0,))
            ).reshape(count, KB, HD)
            if own:
                value_grad[:, :, lanes[g]] = dv
            else:
                back_v[pl.ds(first, count), :, lanes[g]] = dv.astype(BF16)

    early(n, kblocks, True)

    mark("answer")

    def name(j):
        mine = jnp.where(lane == me, asked[j], 0.0)
        named[j] = jnp.broadcast_to(jnp.sum(mine, axis=1, keepdims=True), (8, kv_cols))

    def masks(j):
        return [
            jnp.concatenate([named[j] == w + 1.0] * (KB // 8), axis=0) for w in range(kblocks)
        ]

    def kv_copy(j):
        return remote(
            give.at[j], pool.at[me], out_send.at[0], kv_recv.at[place_of_me(j)], {"kv": j}
        )

    def answer(j):
        name(j)
        hit = masks(j)
        for a in range(2):
            block = jnp.zeros((KB, kv_cols), F32)
            for w in range(kblocks):
                block = jnp.where(hit[w], pool[n + w, a].astype(F32), block)
            give[j, a] = block.astype(BF16)
        kv_copy(j).start()

    def wait_plane(ref, sem, k):
        at = ref.at[pl.ds(k * row, row)]
        pltpu.make_async_copy(at, at, sem.at[k]).wait()

    def wait_peer(ref, sem, q):
        at = ref.at[z * row + q]
        pltpu.make_async_copy(at, at, sem.at[zs + q]).wait()

    def answer_plane(i):
        k = zs - 1 - i
        wait_plane(asked, ask_recv, k)
        loop(0, row, lambda q: answer(k * row + q))

    loop(0, zs - 1 - z, answer_plane)
    for q in reversed(range(1, row)):

        @pl.when(q > r)
        def _():
            wait_peer(asked, ask_recv, q)
            answer(z * row + q)

    mark("norm")
    for d in range(1, tp):

        def forward(k):
            at = norm_via.at[d, k]
            pltpu.make_async_copy(at, at, via_recv.at[d, k]).wait()
            norm_start(d, k, True)

        loop(0, per, forward)
    for d in range(tp):
        loop(0, per, lambda k: norm_start(d, k, False))

    mark("near")

    def bv_copy(i):
        return remote(
            back_v.at[i], got_v.at[me], out_send.at[0], bv_recv.at[place_of_me(i)], {"kv": i}
        )

    def bk_copy(i):
        return remote(
            back_k.at[i], got_k.at[me], out_send.at[0], bk_recv.at[place_of_me(i)], {"kv": i}
        )

    def peers(act, test):
        for q in range(row):

            @pl.when(test(q))
            def _():
                act(q)

    peers(lambda q: wait_peer(pool, kv_recv, q), lambda q: q < r)
    early(z * row, row, False)
    peers(lambda q: bv_copy(z * row + q).start(), lambda q: q < r)

    mark("far")

    def early_plane(i):
        k = z - 1 - i
        wait_plane(pool, kv_recv, k)
        early(k * row, row, False)
        loop(0, row, lambda q: bv_copy(k * row + q).start())

    loop(0, z, early_plane)

    mark("late")
    for g in range(kv_heads):
        delta[g] = jnp.broadcast_to(jnp.sum(delta[g], axis=0, keepdims=True), (8, width))

    def late(first, count, own):
        for g in range(kv_heads):
            for u in range(count):
                ds = p_low[g, first + u].astype(F32) * (dp[g, first + u] - delta[g, :1])
                p_low[g, first + u] = ds.astype(BF16)
            ds = p_low[g, pl.ds(first, count)].reshape(count * KB, width)
            dk = dot(ds, q_all[g], ((1,), (0,))).reshape(count, KB, HD) * scale
            if own:
                key_grad[:, :, lanes[g]] = dk
            else:
                back_k[pl.ds(first, count), :, lanes[g]] = dk.astype(BF16)
            dq = dot(take(0, first, count, g), ds, ((0,), (0,)))
            dq_acc[g] = dq if own else dq_acc[g] + dq

    late(n, kblocks, True)

    def late_plane(i):
        k = z - 1 - i
        late(k * row, row, False)
        loop(0, row, lambda q: bk_copy(k * row + q).start())

    loop(0, z, late_plane)
    late(z * row, row, False)
    peers(lambda q: bk_copy(z * row + q).start(), lambda q: q < r)

    mark("dq")
    for g in range(kv_heads):
        for h in range(group):
            at = (g * group + h) * HD
            query_grad[:, at : at + HD] = dq_acc[g, :, h * tok : (h + 1) * tok].T * scale

    def swap_copy(d, k):
        at = norm_pool.at[col, pl.ds(k * row, row)]
        return remote(at, at, swap_send.at[d], swap_recv.at[d, k], {"tp": (col + d) % tp})

    def swap(k):
        for d in range(1, tp):
            swap_copy(d, k).start()

    def swap_plane(k):
        wait_plane(norm_pool.at[col], norm_recv, k)
        swap(k)

    mark("swap1")
    peers(lambda q: wait_peer(norm_pool.at[col], norm_recv, q), lambda q: q != r)
    swap(z)
    loop(z + 1, zs, swap_plane)

    mark("addv")

    def add(j, got, out):
        hit = masks(j)
        term = got[j].astype(F32)
        for w in range(kblocks):
            out[w] += jnp.where(hit[w], term, 0.0)

    def add_all(got, sem, out):
        def one(q):
            wait_peer(got, sem, q)
            add(z * row + q, got, out)

        peers(one, lambda q: q > r)

        def plane(k):
            wait_plane(got, sem, k)
            loop(0, row, lambda q: add(k * row + q, got, out))

        loop(z + 1, zs, plane)

    add_all(got_v, bv_recv, value_grad)
    low_pool[me] = value_grad[...].reshape(tok, kv_cols).astype(BF16)

    mark("lowstart")

    def low_copy(slot, send, dest):
        return remote(
            low_pool.at[slot], low_pool.at[slot], lo_send.at[send], lo_recv.at[slot], {"kv": dest}
        )

    def low_wait(slot):
        at = low_pool.at[slot]
        pltpu.make_async_copy(at, at, lo_recv.at[slot]).wait()

    def plane_of(k):
        return (z - k + zs) % zs

    loop(1, zs, lambda k: low_copy(me, 0, (z + k) % zs * row + r).start())

    mark("swap2")
    loop(0, z, swap_plane)

    mark("lowrelay")

    def slot_of(k, d, core):
        return plane_of(k) * row + (x + d) % xs * 2 + core

    def across(k, d):
        low_copy(slot_of(k, d, c), 2, z * row + x * 2 + 1 - c).start()

    def relay(k, first):
        if not first:
            low_wait(slot_of(k, 0, c))
        for d in range(1, xs):
            low_copy(slot_of(k, 0, c), 1, z * row + (x + d) % xs * 2 + c).start()
        across(k, 0)

    def cross(k):
        for d in range(1, xs):
            low_wait(slot_of(k, d, c))
            across(k, d)

    def relay_next(k):
        relay(k, False)
        cross(k - 1)

    relay(0, True)
    loop(1, zs, relay_next)
    cross(zs - 1)

    mark("addk")
    add_all(got_k, bk_recv, key_grad)

    mark("product")

    def product(k, first):
        p = plane_of(k)
        for d in range(xs):
            low_wait(slot_of(k, d, 1 - c))
        for d in range(1, tp):
            q = (col + tp - d) % tp
            at = norm_pool.at[q, pl.ds(p * row, row)]
            pltpu.make_async_copy(at, at, swap_recv.at[d, p]).wait()
        v = low_pool[pl.ds(p * row, row)].reshape(row * tok, kv_cols)
        for q in range(tp):
            a = jnp.concatenate([norm_pool[q, p * row + i] for i in range(row)], axis=1)
            w = dot(a, v, ((1,), (0,)))
            if first:
                weight_grad[q * sub : (q + 1) * sub] = w
            else:
                weight_grad[q * sub : (q + 1) * sub] += w

    product(0, True)
    loop(1, zs, lambda k: product(k, False))

    mark("drain")

    def drain(ref, sem):
        pltpu.make_async_copy(ref, ref, sem).wait()

    drain(low_pool.at[pl.ds(0, zs - 1)], lo_send.at[0])
    drain(low_pool.at[pl.ds(0, zs * (xs - 1))], lo_send.at[1])
    drain(low_pool.at[pl.ds(0, zs * xs)], lo_send.at[2])
    drain(give.at[pl.ds(0, n - 1)], out_send.at[0])
    drain(norm_pool.at[0, pl.ds(0, n - 1)], norm_send.at[0])
    for d in range(1, tp):
        drain(norm_parts.at[0], via_send.at[d])
        drain(norm_pool.at[0], swap_send.at[d])
    loop(0, me, lambda i: ask_copy(i).wait_send())
    mark(None)


def finish(*refs):
    count = len(refs) // 2
    sem = refs[-1]
    copies = [
        pltpu.make_async_copy(refs[i], refs[count + i], sem.at[i]) for i in range(count)
    ]
    for cp in copies:
        cp.start()
    for cp in copies:
        cp.wait()


def local(n, tp, queries, keys, values, logsum, out_grad, normed_input, chosen):
    tok, kv_cols = keys.shape
    kv_heads = kv_cols // HD
    heads = queries.shape[1] // HD
    group = heads // kv_heads
    kblocks = tok // KB
    rows = normed_input.shape[1] * tp // n
    row = 2 * tp
    zs = n // row
    width = group * tok
    per = n // tp
    sub = rows // tp
    slots = n + kblocks
    hbm = pl.BlockSpec(memory_space=pltpu.HBM)
    vmem = pl.BlockSpec(memory_space=pltpu.VMEM)
    dma = pltpu.SemaphoreType.DMA
    groups = zs + row
    outs = (
        (tok, queries.shape[1]),
        (kblocks, KB, kv_cols),
        (kblocks, KB, kv_cols),
        (rows, kv_cols),
    )
    held = pl.pallas_call(
        functools.partial(kernel, n, tp),
        out_shape=tuple(pltpu.VMEM(shape, F32) for shape in outs),
        in_specs=[hbm] * 7,
        out_specs=(vmem,) * 4,
        scratch_shapes=[
            pltpu.SMEM(chosen.shape, jnp.int32),
            pltpu.VMEM((kv_heads, width, HD), BF16),
            pltpu.VMEM((kv_heads, width, HD), BF16),
            pltpu.VMEM((heads, tok), F32),
            pltpu.VMEM((kv_heads, 1, width), F32),
            pltpu.VMEM(normed_input.shape, BF16),
            pltpu.VMEM((slots, 2, KB, kv_cols), BF16),
            pltpu.VMEM((8, HD), F32),
            pltpu.VMEM((n, 8, HD), F32),
            pltpu.VMEM((n, 8, kv_cols), F32),
            pltpu.VMEM((n, 2, KB, kv_cols), BF16),
            pltpu.VMEM((n, KB, kv_cols), BF16),
            pltpu.VMEM((n, KB, kv_cols), BF16),
            pltpu.VMEM((n, KB, kv_cols), BF16),
            pltpu.VMEM((n, KB, kv_cols), BF16),
            pltpu.VMEM((n, tok, kv_cols), BF16),
            pltpu.VMEM((tp, per, sub, tok), BF16),
            pltpu.VMEM((tp, per, sub, tok), BF16),
            pltpu.VMEM((tp, n, sub, tok), BF16),
            pltpu.VMEM((HD, tok), F32),
            pltpu.VMEM((HD, tok), F32),
            pltpu.VMEM((max(row, kblocks) * KB, width), F32),
            pltpu.VMEM((kv_heads, slots, KB, width), F32),
            pltpu.VMEM((kv_heads, slots, KB, width), BF16),
            pltpu.VMEM((kv_heads, 8, width), F32),
            pltpu.VMEM((kv_heads, HD, width), F32),
            dma((7,)),
            dma((n,)),
            dma((groups,)),
            dma((1,)),
            dma((groups,)),
            dma((groups,)),
            dma((groups,)),
            dma((tp,)),
            dma((tp, per)),
            dma((1,)),
            dma((groups,)),
            dma((tp,)),
            dma((tp, zs)),
            dma((3,)),
            dma((n,)),
        ],
        compiler_params=pltpu.CompilerParams(
            collective_id=0, has_side_effects=True, vmem_limit_bytes=56 * 1024 * 1024
        ),
        name="attention_back",
    )(
        chosen,
        queries,
        keys.reshape(kblocks, KB, kv_cols),
        values.reshape(kblocks, KB, kv_cols),
        logsum.T,
        out_grad,
        normed_input,
    )
    query_grad, key_grad, value_grad, weight_grad = pl.pallas_call(
        finish,
        out_shape=tuple(jax.ShapeDtypeStruct(shape, F32) for shape in outs),
        in_specs=[vmem] * 4,
        out_specs=(hbm,) * 4,
        scratch_shapes=[dma((4,))],
        compiler_params=pltpu.CompilerParams(vmem_limit_bytes=4 * 1024 * 1024),
        name="write_out",
    )(*held)
    return (
        query_grad,
        key_grad.reshape(tok, kv_cols),
        value_grad.reshape(tok, kv_cols),
        weight_grad,
    )


def solution(mesh):
    n, tp = mesh.shape["kv"], mesh.shape["tp"]
    in_specs = (P("kv", "tp"),) * 6 + (P("kv", None),)
    out_specs = (P("kv", "tp"),) * 4
    return jax.shard_map(
        functools.partial(local, n, tp),
        mesh=mesh,
        in_specs=in_specs,
        out_specs=out_specs,
        check_vma=False,
    )
```

```python
import functools

import jax
import jax.numpy as jnp
from jax import lax
from jax.experimental import pallas as pl
from jax.experimental.pallas import tpu as pltpu
from jax.sharding import PartitionSpec as P

HD = 128
QB = 64
KB = 32
NSEL = 16
FAR = 1e30
LOG2E = 1.4426950408889634

MESH = pl.DeviceIdType.MESH
F32 = jnp.float32
BF16 = jnp.bfloat16


def remote(src, dst, send_sem, recv_sem, device_id):
    return pltpu.make_async_remote_copy(
        src_ref=src,
        dst_ref=dst,
        send_sem=send_sem,
        recv_sem=recv_sem,
        device_id=device_id,
        device_id_type=MESH,
    )


def dot(a, b, dims):
    return lax.dot_general(a, b, (dims, ((), ())), preferred_element_type=F32)


def loop(first, last, body):
    def step(i, carry):
        body(i)
        return carry

    lax.fori_loop(first, last, step, 0)


def kernel(
    n,
    tp,
    chosen_hbm,
    queries,
    keys,
    values,
    logsum,
    out_grad,
    normed_hbm,
    query_grad,
    key_grad,
    value_grad,
    weight_grad,
    chosen,
    q_all,
    do_all,
    logs,
    log2s,
    normed,
    column,
    pool,
    asked,
    named,
    named_in,
    give,
    back_v,
    back_k,
    got_v,
    got_k,
    low_pool,
    norm_parts,
    norm_via,
    norm_pool,
    pen,
    pen_own,
    s_buf,
    dp,
    p_low,
    delta,
    dq_acc,
    in_sem,
    send_sem,
    ask_recv,
    col_recv,
    kv_recv,
    bv_recv,
    bk_recv,
    via_recv,
    norm_recv,
    swap_recv,
    lo_recv,
):
    me = lax.axis_index("kv")
    col = lax.axis_index("tp")
    kblocks = keys.shape[0]
    tok = kblocks * KB
    qblocks = tok // QB
    kv_cols = keys.shape[2]
    kv_heads = kv_cols // HD
    group = queries.shape[1] // kv_cols
    width = group * tok
    per = n // tp
    sub = norm_parts.shape[2]
    rows = sub * tp
    scale = HD ** (-0.5)
    xs = tp
    row = 2 * xs
    zs = n // row
    z = me // row
    r = me % row
    x = r // 2
    c = r % 2
    lanes = [slice(g * HD, (g + 1) * HD) for g in range(kv_heads)]

    barrier = pltpu.get_barrier_semaphore()


    def greet(i):
        pl.semaphore_signal(barrier, inc=1, device_id={"kv": i}, device_id_type=MESH)

    loop(0, n, greet)
    for d in range(1, tp):
        pl.semaphore_signal(
            barrier, inc=1, device_id={"tp": (col + d) % tp}, device_id_type=MESH
        )

    ins = [
        [pltpu.make_async_copy(chosen_hbm, chosen, in_sem.at[0])],
        [pltpu.make_async_copy(normed_hbm, normed, in_sem.at[1])],
        [
            pltpu.make_async_copy(ref.at[:, :, lanes[g]], column.at[z, g, a], in_sem.at[2])
            for a, ref in ((0, keys), (1, values))
            for g in range(kv_heads)
        ],
        [pltpu.make_async_copy(logsum, logs, in_sem.at[3])],
    ]
    big = []
    for a, (src, dst) in enumerate(((queries, q_all), (out_grad, do_all))):
        for g in range(kv_heads):
            for h in range(group):
                at = (g * group + h) * HD
                big.append(
                    pltpu.make_async_copy(
                        src.at[:, at : at + HD],
                        dst.at[g, h * tok : (h + 1) * tok],
                        in_sem.at[4 + a],
                    )
                )
    for cs in ins:
        for cp in cs:
            cp.start()
    for cp in big:
        cp.start()

    for q in range(row):

        @pl.when(q >= r)
        def _():
            pool[z * row + q] = jnp.zeros_like(pool[z * row + q])

    ins[0][0].wait()
    lane = lax.broadcasted_iota(jnp.int32, (8, HD), 1)
    base = lane * kblocks
    wanted = jnp.zeros((8, HD), F32)
    missing = []
    missing_own = []
    for b in range(qblocks):
        far = jnp.full((8, HD), FAR, F32)
        far_own = jnp.full((8, HD), FAR, F32)
        for e in range(NSEL):
            block = chosen[b, e]
            at = block - base
            hit = (at >= 0) & (at < kblocks)
            wanted = jnp.where(hit, (at + 1).astype(F32), wanted)
            far = jnp.where(hit, 0.0, far)
            far_own = jnp.where(block - me * kblocks == lane, 0.0, far_own)
        missing.append(jnp.broadcast_to(far[:1], (QB, HD)))
        missing_own.append(jnp.broadcast_to(far_own[:1], (QB, HD)))
    asked[me] = wanted[:1]
    pen[...] = jnp.concatenate(missing, axis=0).T
    pen_own[...] = jnp.concatenate(missing_own, axis=0).T

    ins[1][0].wait()
    for m in range(normed.shape[1] // HD):
        turned = normed[:, m * HD : (m + 1) * HD].T
        for p in range(0, HD, sub):
            at = m * HD + p
            norm_parts[at % rows // sub, at // rows] = turned[p : p + sub]

    pl.semaphore_wait(barrier, n + tp - 1)

    def place(i):
        return jnp.where(i // row == z, zs + i % row, i // row)


    def ask_copy(i):
        return remote(
            asked.at[me], asked.at[me], send_sem.at[0], ask_recv.at[place_of_me(i)], {"kv": i}
        )

    def place_of_me(i):
        return jnp.where(i // row == z, zs + r, z)

    def column_copy(p, g, a):
        at = column.at[p, g, a]
        return remote(at, at, send_sem.at[1], col_recv.at[p, g, a], {"kv": me + row})

    def climb(p, g, a):
        @pl.when(z + 1 < zs)
        def _():
            column_copy(p, g, a).start()

    for cp in ins[2]:
        cp.wait()
    for g in range(kv_heads):
        for a in range(2):
            climb(z, g, a)
    for d in range(1, row):
        ask_copy(z * row + (r + d) % row).start()
    loop(0, z * row, lambda i: ask_copy(i).start())

    def via_copy(d, k):
        q = (col + d) % tp
        return remote(
            norm_parts.at[q, k], norm_via.at[d, k], send_sem.at[2], via_recv.at[d, k], {"tp": q}
        )

    for d in range(1, tp):
        loop(0, per, lambda k: via_copy(d, k).start())

    def norm_copy(d, k):
        t = (col + tp - d) % tp
        dest = t * per + k
        src = norm_parts.at[col, k] if d == 0 else norm_via.at[d, k]
        return remote(
            src, norm_pool.at[col, me], send_sem.at[3], norm_recv.at[place_of_me(dest)],
            {"kv": dest},
        )

    def norm_start(d, k, low):
        t = (col + tp - d) % tp
        dest = t * per + k

        if low:

            @pl.when(dest == me)
            def _():
                src = norm_parts[col, k] if d == 0 else norm_via[d, k]
                norm_pool[col, me] = src

            @pl.when((dest != me) & (dest // row <= z))
            def _():
                norm_copy(d, k).start()
        else:

            @pl.when(dest // row > z)
            def _():
                norm_copy(d, k).start()

    for cp in ins[3]:
        cp.wait()
    for cp in big:
        cp.wait()
    for g in range(kv_heads):
        log2s[g] = jnp.concatenate(
            [logs[g * group + h : g * group + h + 1] * LOG2E for h in range(group)], axis=1
        )

    def take(a, first, count, g):
        if first is None:
            return column[z, g, a].reshape(count * KB, HD)
        return pool[pl.ds(first, count), g, a].reshape(count * KB, HD)

    key_iota = lax.broadcasted_iota(jnp.int32, (KB, tok), 0)
    row_iota = lax.broadcasted_iota(jnp.int32, (KB, tok), 1)

    def early(first, count, own):
        for g in range(kv_heads):
            s_buf[: count * KB] = dot(take(0, None if own else first, count, g), q_all[g], ((1,), (1,)))
            dp[g, pl.ds(first, count)] = dot(
                take(1, None if own else first, count, g), do_all[g], ((1,), (1,))
            ).reshape(count, KB, width)
            total = jnp.zeros((8, width), F32) if own else delta[g]
            for u in range(count):
                if own:
                    gone = jnp.where(key_iota + u * KB <= row_iota, 0.0, FAR)
                    gone = gone + pen_own[u : u + 1]
                else:
                    gone = pen[pl.ds(first + u, 1)]
                bias = log2s[g] + jnp.concatenate([gone] * group, axis=1)
                p = jnp.exp2(s_buf[u * KB : (u + 1) * KB] * (scale * LOG2E) - bias)
                p_low[g, first + u] = p.astype(BF16)
                pd = p * dp[g, first + u]
                total = total + jnp.sum(pd.reshape(KB // 8, 8, width), axis=0)
            delta[g] = total
            dv = dot(
                p_low[g, pl.ds(first, count)].reshape(count * KB, width), do_all[g], ((1,), (0,))
            ).reshape(count, KB, HD)
            if own:
                value_grad[:, :, lanes[g]] = dv
            else:
                back_v[pl.ds(first, count), :, lanes[g]] = dv.astype(BF16)

    early(n, kblocks, True)


    def spell(v, at):
        mine = jnp.where(lane == at, jnp.broadcast_to(v, (8, HD)), 0.0)
        return jnp.broadcast_to(jnp.sum(mine, axis=1, keepdims=True), (8, HD))

    def masks(v):
        return [jnp.concatenate([v == w + 1.0] * (KB // 8), axis=0) for w in range(kblocks)]

    def wait_plane(ref, sem, k):
        at = ref.at[pl.ds(k * row, row)]
        pltpu.make_async_copy(at, at, sem.at[k]).wait()

    def wait_peer(ref, sem, q):
        at = ref.at[z * row + q]
        pltpu.make_async_copy(at, at, sem.at[zs + q]).wait()

    def peers(act, test):
        for q in range(row):

            @pl.when(test(q))
            def _():
                act(q)

    peers(lambda q: wait_peer(asked, ask_recv, q), lambda q: q != r)

    def spell_plane(p):
        for d in range(row):
            named_in[p, d] = spell(asked[z * row + (r + d) % row], p * row + r)

    loop(0, z + 1, spell_plane)

    def give_copy(p, d):
        return remote(
            give.at[p, d],
            pool.at[p * row + r],
            send_sem.at[4],
            kv_recv.at[p, r],
            {"kv": z * row + (r + d) % row},
        )

    def pick(p, d, g, a, hit):
        block = jnp.zeros((KB, HD), F32)
        for w in range(kblocks):
            block = jnp.where(hit[w], column[p, g, a, w].astype(F32), block)
        return block.astype(BF16)

    def answer(p, d):
        hit = masks(named_in[p, d])
        for g in range(kv_heads):
            for a in range(2):
                block = pick(p, d, g, a, hit)
                if d == 0:
                    pool[p * row + r, g, a] = block
                else:
                    give[p, d, g, a] = block
        if d > 0:
            give_copy(p, d).start()

    for d in range(1, row):

        @pl.when(r + d < row)
        def _():
            answer(z, d)

    def bv_copy(i):
        return remote(
            back_v.at[i], got_v.at[me], send_sem.at[5], bv_recv.at[place_of_me(i)], {"kv": i}
        )

    def bk_copy(i):
        return remote(
            back_k.at[i], got_k.at[me], send_sem.at[6], bk_recv.at[place_of_me(i)], {"kv": i}
        )

    def wait_give(p, q):
        at = pool.at[p * row + q]
        pltpu.make_async_copy(at, at, kv_recv.at[p, q]).wait()

    def near():
        peers(lambda q: wait_give(z, q), lambda q: q < r)
        early(z * row, row, False)
        peers(lambda q: bv_copy(z * row + q).start(), lambda q: q < r)

    def far(p):
        peers(lambda q: wait_give(p, q), lambda q: q != r)
        early(p * row, row, False)
        loop(0, row, lambda q: bv_copy(p * row + q).start())

    def forward(k):
        for d in range(1, tp):
            at = norm_via.at[d, k]
            pltpu.make_async_copy(at, at, via_recv.at[d, k]).wait()
            norm_start(d, k, True)

    share = per // 2
    loop(0, per, lambda k: norm_start(0, k, True))

    def descend(i):
        p = z - 1 - i
        for g in range(kv_heads):
            for a in range(2):
                at = column.at[p, g, a]
                pltpu.make_async_copy(at, at, col_recv.at[p, g, a]).wait()
                climb(p, g, a)
        for d in reversed(range(row)):
            answer(p, d)
        loop(jnp.minimum(i, 2) * share, jnp.minimum(i + 1, 2) * share, forward)

        @pl.when(i == 0)
        def _():
            near()

        @pl.when(i > 0)
        def _():
            far(p + 1)

    loop(0, z, descend)

    @pl.when(z == 0)
    def _():
        near()

    @pl.when(z > 0)
    def _():
        far(0)

    for g in range(kv_heads):
        delta[g] = jnp.broadcast_to(jnp.sum(delta[g], axis=0, keepdims=True), (8, width))

    def late(first, count, own):
        for g in range(kv_heads):
            for u in range(count):
                ds = p_low[g, first + u].astype(F32) * (dp[g, first + u] - delta[g, :1])
                p_low[g, first + u] = ds.astype(BF16)
            ds = p_low[g, pl.ds(first, count)].reshape(count * KB, width)
            dk = dot(ds, q_all[g], ((1,), (0,))).reshape(count, KB, HD) * scale
            if own:
                key_grad[:, :, lanes[g]] = dk
            else:
                back_k[pl.ds(first, count), :, lanes[g]] = dk.astype(BF16)
            dq = dot(take(0, None if own else first, count, g), ds, ((0,), (0,)))
            dq_acc[g] = dq if own else dq_acc[g] + dq

    late(n, kblocks, True)

    def late_plane(i):
        k = z - 1 - i
        late(k * row, row, False)

    loop(0, z, late_plane)
    late(z * row, row, False)

    for g in range(kv_heads):
        for h in range(group):
            at = (g * group + h) * HD
            query_grad[:, at : at + HD] = dq_acc[g, :, h * tok : (h + 1) * tok].T * scale


    def swap_copy(d, k):
        at = norm_pool.at[col, pl.ds(k * row, row)]
        return remote(at, at, send_sem.at[7], swap_recv.at[d, k], {"tp": (col + d) % tp})

    def swap(k):
        for d in range(1, tp):
            swap_copy(d, k).start()

    def swap_plane(k):
        wait_plane(norm_pool.at[col], norm_recv, k)
        swap(k)

    loop(jnp.minimum(z, 2) * share, per, forward)
    for d in range(tp):
        loop(0, per, lambda k: norm_start(d, k, False))


    def name(j):
        named[j] = spell(asked[j], me)

    def name_plane(k):
        wait_plane(asked, ask_recv, k)
        for q in range(row):
            name(k * row + q)

    for q in range(row):
        name(z * row + q)
    loop(z + 1, zs, name_plane)


    def add(j, got, out):
        hit = [jnp.concatenate([m] * kv_heads, axis=1) for m in masks(named[j])]
        term = got[j].astype(F32)
        for w in range(kblocks):
            out[w] += jnp.where(hit[w], term, 0.0)

    def add_near(got, sem, out):
        def one(q):
            wait_peer(got, sem, q)
            add(z * row + q, got, out)

        peers(one, lambda q: q > r)

    def add_far(got, sem, out, first, last):
        def plane(k):
            wait_plane(got, sem, k)
            loop(0, row, lambda q: add(k * row + q, got, out))

        loop(first, last, plane)

    add_near(got_v, bv_recv, value_grad)
    above = jnp.minimum(z + 2, zs)
    add_far(got_v, bv_recv, value_grad, z + 1, above)
    add_far(got_v, bv_recv, value_grad, above, zs)
    low_pool[me] = value_grad[...].reshape(tok, kv_cols).astype(BF16)


    def low_copy(slot, send, dest):
        return remote(
            low_pool.at[slot], low_pool.at[slot], send_sem.at[send], lo_recv.at[slot], {"kv": dest}
        )

    def low_wait(slot):
        at = low_pool.at[slot]
        pltpu.make_async_copy(at, at, lo_recv.at[slot]).wait()

    def up(k):
        return low_copy(me, 8, k * row + r)

    def down(p):
        return low_copy(p * row + r, 9, (z - 1) * row + r)

    loop(0, zs - 1 - z, lambda i: up(zs - 1 - i).start())

    @pl.when(z > 0)
    def _():
        down(z).start()


    def slot_of(p, d, core):
        return p * row + (x + d) % xs * 2 + core

    def across(p, d):
        low_copy(slot_of(p, d, c), 10, z * row + x * 2 + 1 - c).start()

    def spread(p):
        for d in range(1, xs):
            low_copy(slot_of(p, 0, c), 11, z * row + (x + d) % xs * 2 + c).start()
        across(p, 0)

    def cross(p):
        for d in range(1, xs):
            low_wait(slot_of(p, d, c))
            across(p, d)

    def order(k):
        return jnp.where(k < zs - z, z + k, zs - 1 - k)

    spread(z)
    peers(lambda q: wait_peer(norm_pool.at[col], norm_recv, q), lambda q: q != r)
    swap(z)

    def relay(k):
        p = order(k)
        slot = slot_of(p, 0, c)
        swap_plane(p)
        low_wait(slot)

        @pl.when((p > z) & (z > 0))
        def _():
            down(p).start()

        spread(p)
        cross(order(k - 1))

    relay(1)
    loop(0, me, lambda i: bk_copy(i).start())
    loop(2, zs, relay)
    cross(order(zs - 1))

    add_near(got_k, bk_recv, key_grad)
    add_far(got_k, bk_recv, key_grad, z + 1, zs)


    def product(k, first):
        p = order(k)
        for d in range(xs):
            low_wait(slot_of(p, d, 1 - c))
        for d in range(1, tp):
            q = (col + tp - d) % tp
            at = norm_pool.at[q, pl.ds(p * row, row)]
            pltpu.make_async_copy(at, at, swap_recv.at[d, p]).wait()
        v = low_pool[pl.ds(p * row, row)].reshape(row * tok, kv_cols)
        for q in range(tp):
            a = jnp.concatenate([norm_pool[q, p * row + i] for i in range(row)], axis=1)
            w = dot(a, v, ((1,), (0,)))
            if first:
                weight_grad[q * sub : (q + 1) * sub] = w
            else:
                weight_grad[q * sub : (q + 1) * sub] += w

    product(0, True)
    loop(1, zs, lambda k: product(k, False))


    def drain(ref, sem):
        pltpu.make_async_copy(ref, ref, sem).wait()

    drain(low_pool.at[pl.ds(0, zs * xs)], send_sem.at[10])
    drain(low_pool.at[pl.ds(0, zs * (xs - 1))], send_sem.at[11])
    drain(norm_pool.at[0, pl.ds(0, n - 1)], send_sem.at[3])
    for d in range(1, tp):
        drain(norm_parts.at[0], send_sem.at[2])
        drain(norm_pool.at[0], send_sem.at[7])
    loop(z + 1, zs, lambda k: up(k).wait_send())

    @pl.when(z > 0)
    def _():
        loop(z, zs, lambda p: down(p).wait_send())

    for d in range(1, row):
        ask_copy(z * row + (r + d) % row).wait_send()

        @pl.when(r + d < row)
        def _():
            give_copy(z, d).wait_send()

    def drain_plane(p):
        for d in range(1, row):
            give_copy(p, d).wait_send()

    def drain_column(p):
        for g in range(kv_heads):
            for a in range(2):
                column_copy(p, g, a).wait_send()

    def drain_back(i):
        bv_copy(i).wait_send()
        bk_copy(i).wait_send()

    loop(0, z, drain_plane)
    loop(0, z * row, lambda i: ask_copy(i).wait_send())
    loop(0, me, drain_back)

    @pl.when(z + 1 < zs)
    def _():
        loop(0, z + 1, drain_column)


def finish(*refs):
    count = len(refs) // 2
    sem = refs[-1]
    copies = [
        pltpu.make_async_copy(refs[i], refs[count + i], sem.at[i]) for i in range(count)
    ]
    for cp in copies:
        cp.start()
    for cp in copies:
        cp.wait()


def local(n, tp, queries, keys, values, logsum, out_grad, normed_input, chosen):
    tok, kv_cols = keys.shape
    kv_heads = kv_cols // HD
    heads = queries.shape[1] // HD
    group = heads // kv_heads
    kblocks = tok // KB
    rows = normed_input.shape[1] * tp // n
    row = 2 * tp
    zs = n // row
    width = group * tok
    per = n // tp
    sub = rows // tp
    slots = n + kblocks
    hbm = pl.BlockSpec(memory_space=pltpu.HBM)
    vmem = pl.BlockSpec(memory_space=pltpu.VMEM)
    dma = pltpu.SemaphoreType.DMA
    groups = zs + row
    outs = (
        (tok, queries.shape[1]),
        (kblocks, KB, kv_cols),
        (kblocks, KB, kv_cols),
        (rows, kv_cols),
    )
    held = pl.pallas_call(
        functools.partial(kernel, n, tp),
        out_shape=tuple(pltpu.VMEM(shape, F32) for shape in outs),
        in_specs=[hbm] * 7,
        out_specs=(vmem,) * 4,
        scratch_shapes=[
            pltpu.SMEM(chosen.shape, jnp.int32),
            pltpu.VMEM((kv_heads, width, HD), BF16),
            pltpu.VMEM((kv_heads, width, HD), BF16),
            pltpu.VMEM((heads, tok), F32),
            pltpu.VMEM((kv_heads, 1, width), F32),
            pltpu.VMEM(normed_input.shape, BF16),
            pltpu.VMEM((zs, kv_heads, 2, kblocks, KB, HD), BF16),
            pltpu.VMEM((n, kv_heads, 2, KB, HD), BF16),
            pltpu.VMEM((n, 1, HD), F32),
            pltpu.VMEM((n, 8, HD), F32),
            pltpu.VMEM((zs, row, 8, HD), F32),
            pltpu.VMEM((zs, row, kv_heads, 2, KB, HD), BF16),
            pltpu.VMEM((n, KB, kv_cols), BF16),
            pltpu.VMEM((n, KB, kv_cols), BF16),
            pltpu.VMEM((n, KB, kv_cols), BF16),
            pltpu.VMEM((n, KB, kv_cols), BF16),
            pltpu.VMEM((n, tok, kv_cols), BF16),
            pltpu.VMEM((tp, per, sub, tok), BF16),
            pltpu.VMEM((tp, per, sub, tok), BF16),
            pltpu.VMEM((tp, n, sub, tok), BF16),
            pltpu.VMEM((HD, tok), F32),
            pltpu.VMEM((HD, tok), F32),
            pltpu.VMEM((max(row, kblocks) * KB, width), F32),
            pltpu.VMEM((kv_heads, slots, KB, width), F32),
            pltpu.VMEM((kv_heads, slots, KB, width), BF16),
            pltpu.VMEM((kv_heads, 8, width), F32),
            pltpu.VMEM((kv_heads, HD, width), F32),
            dma((6,)),
            dma((12,)),
            dma((groups,)),
            dma((zs, kv_heads, 2)),
            dma((zs, row)),
            dma((groups,)),
            dma((groups,)),
            dma((tp, per)),
            dma((groups,)),
            dma((tp, zs)),
            dma((n,)),
        ],
        compiler_params=pltpu.CompilerParams(
            collective_id=0, has_side_effects=True, vmem_limit_bytes=56 * 1024 * 1024
        ),
        name="attention_back",
    )(
        chosen,
        queries,
        keys.reshape(kblocks, KB, kv_cols),
        values.reshape(kblocks, KB, kv_cols),
        logsum.T,
        out_grad,
        normed_input,
    )
    query_grad, key_grad, value_grad, weight_grad = pl.pallas_call(
        finish,
        out_shape=tuple(jax.ShapeDtypeStruct(shape, F32) for shape in outs),
        in_specs=[vmem] * 4,
        out_specs=(hbm,) * 4,
        scratch_shapes=[dma((4,))],
        compiler_params=pltpu.CompilerParams(vmem_limit_bytes=4 * 1024 * 1024),
        name="write_out",
    )(*held)
    return (
        query_grad,
        key_grad.reshape(tok, kv_cols),
        value_grad.reshape(tok, kv_cols),
        weight_grad,
    )


def solution(mesh):
    n, tp = mesh.shape["kv"], mesh.shape["tp"]
    in_specs = (P("kv", "tp"),) * 6 + (P("kv", None),)
    out_specs = (P("kv", "tp"),) * 4
    return jax.shard_map(
        functools.partial(local, n, tp),
        mesh=mesh,
        in_specs=in_specs,
        out_specs=out_specs,
        check_vma=False,
    )
```

```python
import functools

import jax
import jax.numpy as jnp
from jax import lax
from jax.experimental import pallas as pl
from jax.experimental.pallas import tpu as pltpu
from jax.sharding import PartitionSpec as P

HD = 128
QB = 64
KB = 32
NSEL = 16
FAR = 1e30
EARLY2 = 8
EARLY = 6
EARLY1 = 4
LOG2E = 1.4426950408889634

MESH = pl.DeviceIdType.MESH
F32 = jnp.float32
BF16 = jnp.bfloat16


def remote(src, dst, send_sem, recv_sem, device_id):
    return pltpu.make_async_remote_copy(
        src_ref=src,
        dst_ref=dst,
        send_sem=send_sem,
        recv_sem=recv_sem,
        device_id=device_id,
        device_id_type=MESH,
    )


def dot(a, b, dims):
    return lax.dot_general(a, b, (dims, ((), ())), preferred_element_type=F32)


def loop(first, last, body):
    def step(i, carry):
        body(i)
        return carry

    lax.fori_loop(first, last, step, 0)


def kernel(
    n,
    tp,
    chosen_hbm,
    queries,
    keys,
    values,
    logsum,
    out_grad,
    normed_hbm,
    query_grad,
    key_grad,
    value_grad,
    weight_grad,
    chosen,
    q_all,
    do_all,
    logs,
    log2s,
    normed,
    column,
    pool,
    asked,
    named,
    named_in,
    give,
    back_v,
    back_k,
    got_v,
    got_k,
    low_pool,
    norm_parts,
    norm_via,
    norm_pool,
    pen,
    pen_own,
    s_buf,
    dp,
    p_low,
    delta,
    dq_acc,
    in_sem,
    send_sem,
    ask_recv,
    col_recv,
    kv_recv,
    bv_recv,
    bk_recv,
    via_recv,
    norm_recv,
    swap_recv,
    lo_recv,
):
    me = lax.axis_index("kv")
    col = lax.axis_index("tp")
    kblocks = keys.shape[0]
    tok = kblocks * KB
    qblocks = tok // QB
    kv_cols = keys.shape[2]
    kv_heads = kv_cols // HD
    group = queries.shape[1] // kv_cols
    width = group * tok
    per = n // tp
    sub = norm_parts.shape[2]
    rows = sub * tp
    scale = HD ** (-0.5)
    xs = tp
    row = 2 * xs
    zs = n // row
    z = me // row
    r = me % row
    x = r // 2
    c = r % 2
    lanes = [slice(g * HD, (g + 1) * HD) for g in range(kv_heads)]

    barrier = pltpu.get_barrier_semaphore()


    def greet(i):
        pl.semaphore_signal(barrier, inc=1, device_id={"kv": i}, device_id_type=MESH)

    loop(0, n, greet)
    for d in range(1, tp):
        pl.semaphore_signal(
            barrier, inc=1, device_id={"tp": (col + d) % tp}, device_id_type=MESH
        )

    ins = [
        [pltpu.make_async_copy(chosen_hbm, chosen, in_sem.at[0])],
        [pltpu.make_async_copy(normed_hbm, normed, in_sem.at[1])],
        [
            pltpu.make_async_copy(ref.at[:, :, lanes[g]], column.at[z, g, a], in_sem.at[2])
            for a, ref in ((0, keys), (1, values))
            for g in range(kv_heads)
        ],
        [pltpu.make_async_copy(logsum, logs, in_sem.at[3])],
    ]
    big = []
    for a, (src, dst) in enumerate(((queries, q_all), (out_grad, do_all))):
        for g in range(kv_heads):
            for h in range(group):
                at = (g * group + h) * HD
                big.append(
                    pltpu.make_async_copy(
                        src.at[:, at : at + HD],
                        dst.at[g, h * tok : (h + 1) * tok],
                        in_sem.at[3],
                    )
                )
    for cs in ins:
        for cp in cs:
            cp.start()
    for cp in big:
        cp.start()

    for q in range(row):

        @pl.when(q >= r)
        def _():
            pool[z * row + q] = jnp.zeros_like(pool[z * row + q])

    ins[0][0].wait()
    lane = lax.broadcasted_iota(jnp.int32, (8, HD), 1)
    base = lane * kblocks
    wanted = jnp.zeros((8, HD), F32)
    missing = []
    missing_own = []
    for b in range(qblocks):
        far = jnp.full((8, HD), FAR, F32)
        far_own = jnp.full((8, HD), FAR, F32)
        for e in range(NSEL):
            block = chosen[b, e]
            at = block - base
            hit = (at >= 0) & (at < kblocks)
            wanted = jnp.where(hit, (at + 1).astype(F32), wanted)
            far = jnp.where(hit, 0.0, far)
            far_own = jnp.where(block - me * kblocks == lane, 0.0, far_own)
        missing.append(jnp.broadcast_to(far[:1], (QB, HD)))
        missing_own.append(jnp.broadcast_to(far_own[:1], (QB, HD)))
    asked[me] = wanted[:1]
    pen[...] = jnp.concatenate(missing, axis=0).T
    pen_own[...] = jnp.concatenate(missing_own, axis=0).T

    ins[1][0].wait()
    for m in range(normed.shape[1] // HD):
        turned = normed[:, m * HD : (m + 1) * HD].T
        for p in range(0, HD, sub):
            at = m * HD + p
            norm_parts[at % rows // sub, at // rows] = turned[p : p + sub]

    pl.semaphore_wait(barrier, n + tp - 1)

    def place(i):
        return jnp.where(i // row == z, zs + i % row, i // row)


    def ask_copy(i):
        return remote(
            asked.at[me], asked.at[me], send_sem.at[0], ask_recv.at[place_of_me(i)], {"kv": i}
        )

    def place_of_me(i):
        return jnp.where(i // row == z, zs + r, z)

    def column_copy(p, g, a):
        at = column.at[p, g, a]
        return remote(at, at, send_sem.at[0], col_recv.at[p, g, a], {"kv": me + row})

    def climb(p, g, a):
        @pl.when(z + 1 < zs)
        def _():
            column_copy(p, g, a).start()

    for cp in ins[2]:
        cp.wait()
    for g in range(kv_heads):
        for a in range(2):
            climb(z, g, a)
    for d in range(1, row):
        ask_copy(z * row + (r + d) % row).start()
    loop(0, z * row, lambda i: ask_copy(i).start())

    def via_copy(d, k):
        q = (col + d) % tp
        return remote(
            norm_parts.at[q, k], norm_via.at[d, k], send_sem.at[0], via_recv.at[d - 1, k], {"tp": q}
        )

    for d in range(1, tp):
        loop(0, per, lambda k: via_copy(d, k).start())

    def norm_copy(d, k):
        t = (col + tp - d) % tp
        dest = t * per + k
        src = norm_parts.at[col, k] if d == 0 else norm_via.at[d, k]
        return remote(
            src, norm_pool.at[col, me], send_sem.at[0], norm_recv.at[place_of_me(dest)],
            {"kv": dest},
        )

    def norm_start(d, k, low):
        t = (col + tp - d) % tp
        dest = t * per + k

        if low:

            @pl.when(dest == me)
            def _():
                src = norm_parts[col, k] if d == 0 else norm_via[d, k]
                norm_pool[col, me] = src

            @pl.when((dest != me) & (dest // row <= z))
            def _():
                norm_copy(d, k).start()
        else:

            @pl.when(dest // row > z)
            def _():
                norm_copy(d, k).start()

    for cp in ins[3]:
        cp.wait()
    for cp in big:
        cp.wait()
    for g in range(kv_heads):
        log2s[g] = jnp.concatenate(
            [logs[g * group + h : g * group + h + 1] * LOG2E for h in range(group)], axis=1
        )

    def take(a, first, count, g):
        if first is None:
            return column[z, g, a].reshape(count * KB, HD)
        return pool[pl.ds(first, count), g, a].reshape(count * KB, HD)

    key_iota = lax.broadcasted_iota(jnp.int32, (KB, tok), 0)
    row_iota = lax.broadcasted_iota(jnp.int32, (KB, tok), 1)

    def early(first, count, own):
        for g in range(kv_heads):
            s_buf[: count * KB] = dot(take(0, None if own else first, count, g), q_all[g], ((1,), (1,)))
            dp[g, pl.ds(first, count)] = dot(
                take(1, None if own else first, count, g), do_all[g], ((1,), (1,))
            ).reshape(count, KB, width)
            total = jnp.zeros((8, width), F32) if own else delta[g]
            for u in range(count):
                if own:
                    gone = jnp.where(key_iota + u * KB <= row_iota, 0.0, FAR)
                    gone = gone + pen_own[u : u + 1]
                else:
                    gone = pen[pl.ds(first + u, 1)]
                bias = log2s[g] + jnp.concatenate([gone] * group, axis=1)
                p = jnp.exp2(s_buf[u * KB : (u + 1) * KB] * (scale * LOG2E) - bias)
                p_low[g, first + u] = p.astype(BF16)
                pd = p * dp[g, first + u]
                total = total + jnp.sum(pd.reshape(KB // 8, 8, width), axis=0)
            delta[g] = total
            dv = dot(
                p_low[g, pl.ds(first, count)].reshape(count * KB, width), do_all[g], ((1,), (0,))
            ).reshape(count, KB, HD)
            if own:
                value_grad[:, :, lanes[g]] = dv
            else:
                back_v[pl.ds(first, count), :, lanes[g]] = dv.astype(BF16)

    early(n, kblocks, True)


    def spell(v, at):
        mine = jnp.where(lane == at, jnp.broadcast_to(v, (8, HD)), 0.0)
        return jnp.broadcast_to(jnp.sum(mine, axis=1, keepdims=True), (8, HD))

    def masks(v):
        return [jnp.concatenate([v == w + 1.0] * (KB // 8), axis=0) for w in range(kblocks)]

    def wait_plane(ref, sem, k):
        at = ref.at[pl.ds(k * row, row)]
        pltpu.make_async_copy(at, at, sem.at[k]).wait()

    def wait_peer(ref, sem, q):
        at = ref.at[z * row + q]
        pltpu.make_async_copy(at, at, sem.at[zs + q]).wait()

    def peers(act, test):
        for q in range(row):

            @pl.when(test(q))
            def _():
                act(q)

    peers(lambda q: wait_peer(asked, ask_recv, q), lambda q: q != r)

    def spell_plane(p):
        for d in range(row):
            named_in[p, d] = spell(asked[z * row + (r + d) % row], p * row + r)

    loop(0, z + 1, spell_plane)

    def give_copy(p, d):
        return remote(
            give.at[p, d],
            pool.at[p * row + r],
            send_sem.at[0],
            kv_recv.at[p, r],
            {"kv": z * row + (r + d) % row},
        )

    def pick(p, d, g, a, hit):
        block = jnp.zeros((KB, HD), F32)
        for w in range(kblocks):
            block = jnp.where(hit[w], column[p, g, a, w].astype(F32), block)
        return block.astype(BF16)

    def answer(p, d):
        hit = masks(named_in[p, d])
        for g in range(kv_heads):
            for a in range(2):
                block = pick(p, d, g, a, hit)
                if d == 0:
                    pool[p * row + r, g, a] = block
                else:
                    give[p, d, g, a] = block
        if d > 0:
            give_copy(p, d).start()

    for d in range(1, row):

        @pl.when(r + d < row)
        def _():
            answer(z, d)

    def bv_copy(i):
        return remote(
            back_v.at[i], got_v.at[me], send_sem.at[0], bv_recv.at[place_of_me(i)], {"kv": i}
        )

    def bk_copy(i):
        return remote(
            back_k.at[i], got_k.at[me], send_sem.at[0], bk_recv.at[place_of_me(i)], {"kv": i}
        )

    def wait_give(p, q):
        at = pool.at[p * row + q]
        pltpu.make_async_copy(at, at, kv_recv.at[p, q]).wait()

    def near():
        peers(lambda q: wait_give(z, q), lambda q: q < r)
        early(z * row, row, False)
        peers(lambda q: bv_copy(z * row + q).start(), lambda q: q < r)

    def far(p):
        peers(lambda q: wait_give(p, q), lambda q: q != r)
        early(p * row, row, False)
        loop(0, row, lambda q: bv_copy(p * row + q).start())

    def forward(k):
        for d in range(1, tp):
            at = norm_via.at[d, k]
            pltpu.make_async_copy(at, at, via_recv.at[d - 1, k]).wait()

            @pl.when(k < share)
            def _():
                norm_start(d, k, True)

    soon = jnp.where(col == 0, per * EARLY // 8, per * EARLY1 // 8)
    soon2 = per * EARLY2 // 8
    share = jnp.where(z == zs - 1, soon, jnp.where(z == zs - 2, soon2, per))
    half = per // 2

    def begin(i):
        return jnp.minimum(i, 2) * half

    loop(0, share, lambda k: norm_start(0, k, True))

    def descend(i):
        p = z - 1 - i
        for g in range(kv_heads):
            for a in range(2):
                at = column.at[p, g, a]
                pltpu.make_async_copy(at, at, col_recv.at[p, g, a]).wait()
                climb(p, g, a)
        for d in reversed(range(row)):
            answer(p, d)
        loop(begin(i), begin(i + 1), forward)

        @pl.when(i == 0)
        def _():
            near()

        @pl.when(i > 0)
        def _():
            far(p + 1)

    loop(0, z, descend)
    steep = (z == zs - 2) & (z > 0)

    def norm_up():
        for d in range(tp):
            loop(0, per, lambda k: norm_start(d, k, False))

    @pl.when(steep)
    def _():
        norm_up()

    @pl.when(z == 0)
    def _():
        near()

    @pl.when(z > 0)
    def _():
        far(0)

    def late(first, count, own):
        for g in range(kv_heads):
            for u in range(count):
                ds = p_low[g, first + u].astype(F32) * (dp[g, first + u] - delta[g, :1])
                p_low[g, first + u] = ds.astype(BF16)
            ds = p_low[g, pl.ds(first, count)].reshape(count * KB, width)
            dk = dot(ds, q_all[g], ((1,), (0,))).reshape(count, KB, HD) * scale
            if own:
                key_grad[:, :, lanes[g]] = dk
            else:
                back_k[pl.ds(first, count), :, lanes[g]] = dk.astype(BF16)
            dq = dot(take(0, None if own else first, count, g), ds, ((0,), (0,)))
            dq_acc[g] = dq if own else dq_acc[g] + dq

    def late_plane(i):
        k = z - 1 - i
        late(k * row, row, False)

    def swap_copy(d, k):
        at = norm_pool.at[col, pl.ds(k * row, row)]
        return remote(at, at, send_sem.at[0], swap_recv.at[d - 1, k], {"tp": (col + d) % tp})

    def swap(k):
        for d in range(1, tp):
            swap_copy(d, k).start()

    def swap_plane(k):
        wait_plane(norm_pool.at[col], norm_recv, k)
        swap(k)

    def name(j):
        named[j] = spell(asked[j], me)

    def name_plane(k):
        wait_plane(asked, ask_recv, k)
        for q in range(row):
            name(k * row + q)

    def add(j, got, out):
        hit = [jnp.concatenate([m] * kv_heads, axis=1) for m in masks(named[j])]
        term = got[j].astype(F32)
        for w in range(kblocks):
            out[w] += jnp.where(hit[w], term, 0.0)

    def add_near(got, sem, out):
        def one(q):
            wait_peer(got, sem, q)
            add(z * row + q, got, out)

        peers(one, lambda q: q > r)

    def add_far(got, sem, out, first, last):
        def plane(k):
            wait_plane(got, sem, k)
            loop(0, row, lambda q: add(k * row + q, got, out))

        loop(first, last, plane)

    def swap_own():
        peers(lambda q: wait_peer(norm_pool.at[col], norm_recv, q), lambda q: q != r)
        swap(z)

    at = me % per
    ready = jnp.where(at >= soon2, zs - 2, jnp.where(at >= soon, zs - 1, zs))
    ready = jnp.maximum(jnp.minimum(ready, zs), z + 1)
    def low_copy(slot, send, dest):
        return remote(
            low_pool.at[slot], low_pool.at[slot], send_sem.at[0], lo_recv.at[slot], {"kv": dest}
        )

    def low_wait(slot):
        at = low_pool.at[slot]
        pltpu.make_async_copy(at, at, lo_recv.at[slot]).wait()

    def up(k):
        return low_copy(me, 8, k * row + r)

    def down(p):
        return low_copy(p * row + r, 9, (z - 1) * row + r)


    def slot_of(p, d, core):
        return p * row + (x + d) % xs * 2 + core

    def across(p, d):
        low_copy(slot_of(p, d, c), 10, z * row + x * 2 + 1 - c).start()

    def spread(p):
        for d in range(1, xs):
            low_copy(slot_of(p, 0, c), 11, z * row + (x + d) % xs * 2 + c).start()
        across(p, 0)

    def cross(p):
        for d in range(1, xs):
            low_wait(slot_of(p, d, c))
            across(p, d)

    def order(k):
        return jnp.where(k < zs - z, z + k, zs - 1 - k)

    def finish_keys():
        for g in range(kv_heads):
            total = jnp.sum(delta[g], axis=0, keepdims=True)
            delta[g] = jnp.broadcast_to(total, (8, width))
        late(n, kblocks, True)
        loop(0, z, late_plane)
        late(z * row, row, False)
        for g in range(kv_heads):
            for h in range(group):
                at = (g * group + h) * HD
                query_grad[:, at : at + HD] = dq_acc[g, :, h * tok : (h + 1) * tok].T * scale
        loop(begin(z), per, forward)
        for d in range(tp):
            loop(share, per, lambda k: norm_start(d, k, True))

        @pl.when(jnp.logical_not(steep))
        def _():
            norm_up()

    def finish_values():
        for q in range(row):
            name(z * row + q)
        loop(z + 1, zs, name_plane)
        @pl.when(z < zs - 1)
        def _():
            swap_own()
        loop(z + 1, ready, swap_plane)
        add_near(got_v, bv_recv, value_grad)
        above = jnp.minimum(z + 2, zs)
        add_far(got_v, bv_recv, value_grad, z + 1, above)
        add_far(got_v, bv_recv, value_grad, above, zs)
        low_pool[me] = value_grad[...].reshape(tok, kv_cols).astype(BF16)
        loop(0, zs - 1 - z, lambda i: up(zs - 1 - i).start())

        @pl.when(z > 0)
        def _():
            down(z).start()
        spread(z)

    turn = jnp.where(z >= zs - 2, 0, 1)

    def finish_both(i):
        @pl.when(i == turn)
        def _():
            finish_values()

        @pl.when(i == 1 - turn)
        def _():
            finish_keys()

    loop(0, 2, finish_both)

    @pl.when(z == zs - 1)
    def _():
        swap_own()

    def relay(k):
        p = order(k)
        slot = slot_of(p, 0, c)

        @pl.when(p < z)
        def _():
            swap_plane(p)

        low_wait(slot)

        @pl.when((p > z) & (z > 0))
        def _():
            down(p).start()

        spread(p)

    def product(k, first):
        p = order(k)
        for d in range(xs):
            low_wait(slot_of(p, d, 1 - c))
        for d in range(1, tp):
            q = (col + tp - d) % tp
            at = norm_pool.at[q, pl.ds(p * row, row)]
            pltpu.make_async_copy(at, at, swap_recv.at[d - 1, p]).wait()
        v = low_pool[pl.ds(p * row, row)].reshape(row * tok, kv_cols)
        for q in range(tp):
            a = jnp.concatenate([norm_pool[q, p * row + i] for i in range(row)], axis=1)
            w = dot(a, v, ((1,), (0,)))
            if first:
                weight_grad[q * sub : (q + 1) * sub] = w
            else:
                weight_grad[q * sub : (q + 1) * sub] += w

    for k in range(1, zs):
        relay(k)
        if k > 1:
            cross(order(k - 2))
        if k == 1:
            loop(0, me, lambda i: bk_copy(i).start())

        if k == 1:
            loop(ready, zs, swap_plane)

    product(0, True)
    cross(order(zs - 2))
    for k in range(1, zs - 2):
        product(k, False)
    cross(order(zs - 1))
    add_near(got_k, bk_recv, key_grad)
    add_far(got_k, bk_recv, key_grad, z + 1, zs)
    for k in range(max(zs - 2, 1), zs):
        product(k, False)


    def drain(ref, sem):
        pltpu.make_async_copy(ref, ref, sem).wait()

    drain(low_pool.at[pl.ds(0, zs * xs)], send_sem.at[0])
    drain(low_pool.at[pl.ds(0, zs * (xs - 1))], send_sem.at[0])
    drain(norm_pool.at[0, pl.ds(0, n - 1)], send_sem.at[0])
    for d in range(1, tp):
        drain(norm_parts.at[0], send_sem.at[0])
        drain(norm_pool.at[0], send_sem.at[0])
    loop(z + 1, zs, lambda k: up(k).wait_send())

    @pl.when(z > 0)
    def _():
        loop(z, zs, lambda p: down(p).wait_send())

    for d in range(1, row):
        ask_copy(z * row + (r + d) % row).wait_send()

        @pl.when(r + d < row)
        def _():
            give_copy(z, d).wait_send()

    def drain_plane(p):
        for d in range(1, row):
            give_copy(p, d).wait_send()

    def drain_column(p):
        for g in range(kv_heads):
            for a in range(2):
                column_copy(p, g, a).wait_send()

    def drain_back(i):
        bv_copy(i).wait_send()
        bk_copy(i).wait_send()

    loop(0, z, drain_plane)
    loop(0, z * row, lambda i: ask_copy(i).wait_send())
    loop(0, me, drain_back)

    @pl.when(z + 1 < zs)
    def _():
        loop(0, z + 1, drain_column)


def finish(*refs):
    count = len(refs) // 2
    sem = refs[-1]
    copies = [
        pltpu.make_async_copy(refs[i], refs[count + i], sem.at[i]) for i in range(count)
    ]
    for cp in copies:
        cp.start()
    for cp in copies:
        cp.wait()


def local(n, tp, queries, keys, values, logsum, out_grad, normed_input, chosen):
    tok, kv_cols = keys.shape
    kv_heads = kv_cols // HD
    heads = queries.shape[1] // HD
    group = heads // kv_heads
    kblocks = tok // KB
    rows = normed_input.shape[1] * tp // n
    row = 2 * tp
    zs = n // row
    width = group * tok
    per = n // tp
    sub = rows // tp
    slots = n + kblocks
    hbm = pl.BlockSpec(memory_space=pltpu.HBM)
    vmem = pl.BlockSpec(memory_space=pltpu.VMEM)
    dma = pltpu.SemaphoreType.DMA
    groups = zs + row
    outs = (
        (tok, queries.shape[1]),
        (kblocks, KB, kv_cols),
        (kblocks, KB, kv_cols),
        (rows, kv_cols),
    )
    held = pl.pallas_call(
        functools.partial(kernel, n, tp),
        out_shape=tuple(pltpu.VMEM(shape, F32) for shape in outs),
        in_specs=[hbm] * 7,
        out_specs=(vmem,) * 4,
        scratch_shapes=[
            pltpu.SMEM(chosen.shape, jnp.int32),
            pltpu.VMEM((kv_heads, width, HD), BF16),
            pltpu.VMEM((kv_heads, width, HD), BF16),
            pltpu.VMEM((heads, tok), F32),
            pltpu.VMEM((kv_heads, 1, width), F32),
            pltpu.VMEM(normed_input.shape, BF16),
            pltpu.VMEM((zs, kv_heads, 2, kblocks, KB, HD), BF16),
            pltpu.VMEM((n, kv_heads, 2, KB, HD), BF16),
            pltpu.VMEM((n, 1, HD), F32),
            pltpu.VMEM((n, 8, HD), F32),
            pltpu.VMEM((zs, row, 8, HD), F32),
            pltpu.VMEM((zs, row, kv_heads, 2, KB, HD), BF16),
            pltpu.VMEM((n, KB, kv_cols), BF16),
            pltpu.VMEM((n, KB, kv_cols), BF16),
            pltpu.VMEM((n, KB, kv_cols), BF16),
            pltpu.VMEM((n, KB, kv_cols), BF16),
            pltpu.VMEM((n, tok, kv_cols), BF16),
            pltpu.VMEM((tp, per, sub, tok), BF16),
            pltpu.VMEM((tp, per, sub, tok), BF16),
            pltpu.VMEM((tp, n, sub, tok), BF16),
            pltpu.VMEM((HD, tok), F32),
            pltpu.VMEM((HD, tok), F32),
            pltpu.VMEM((max(row, kblocks) * KB, width), F32),
            pltpu.VMEM((kv_heads, slots, KB, width), F32),
            pltpu.VMEM((kv_heads, slots, KB, width), BF16),
            pltpu.VMEM((kv_heads, 8, width), F32),
            pltpu.VMEM((kv_heads, HD, width), F32),
            dma((4,)),
            dma((1,)),
            dma((groups,)),
            dma((zs, kv_heads, 2)),
            dma((zs, row)),
            dma((groups,)),
            dma((groups,)),
            dma((tp - 1, per)),
            dma((groups,)),
            dma((tp - 1, zs)),
            dma((n,)),
        ],
        compiler_params=pltpu.CompilerParams(
            collective_id=0, has_side_effects=True, vmem_limit_bytes=56 * 1024 * 1024
        ),
        name="attention_back",
    )(
        chosen,
        queries,
        keys.reshape(kblocks, KB, kv_cols),
        values.reshape(kblocks, KB, kv_cols),
        logsum.T,
        out_grad,
        normed_input,
    )
    query_grad, key_grad, value_grad, weight_grad = pl.pallas_call(
        finish,
        out_shape=tuple(jax.ShapeDtypeStruct(shape, F32) for shape in outs),
        in_specs=[vmem] * 4,
        out_specs=(hbm,) * 4,
        scratch_shapes=[dma((4,))],
        compiler_params=pltpu.CompilerParams(vmem_limit_bytes=4 * 1024 * 1024),
        name="write_out",
    )(*held)
    return (
        query_grad,
        key_grad.reshape(tok, kv_cols),
        value_grad.reshape(tok, kv_cols),
        weight_grad,
    )


def solution(mesh):
    n, tp = mesh.shape["kv"], mesh.shape["tp"]
    in_specs = (P("kv", "tp"),) * 6 + (P("kv", None),)
    out_specs = (P("kv", "tp"),) * 4
    return jax.shard_map(
        functools.partial(local, n, tp),
        mesh=mesh,
        in_specs=in_specs,
        out_specs=out_specs,
        check_vma=False,
    )
```
